32 devices in a mesh: sp: 8 (over z, y), tp: 4 (over x, core).
Axes of the slice: x: 2, y: 2, z: 4, core: 2. Of those that a mesh axis runs over, the one named last changes fastest.
Arguments:
- tokens: bfloat16 [3072, 2048], P(('sp', 'tp')), may hold values from -8 to 8, as said below
- query_weight: bfloat16 [2048, 1024], P(None, 'tp'), as said below
- key_weight: bfloat16 [2048, 256], P(None, 'tp'), as said below
- value_weight: bfloat16 [2048, 256], P(None, 'tp'), may hold values from -0.125 to 0.125
- out_weight: bfloat16 [1024, 2048], P('tp'), may hold values from -0.75 to 0.75
- query_gain: bfloat16 [16, 64], P('tp'), may hold values from 0.5 to 6.5
- key_gain: bfloat16 [4, 64], P('tp'), may hold values from 0.5 to 6.5
Outputs:
- mixed: bfloat16 [3072, 2048], P(('sp', 'tp'))
- log_sums: float32 [16, 3072], P('tp', 'sp')
The draws below stay inside these ranges and needn't reach their ends.
Inputs may be any that keep to these rules, and one draw needn't show every extreme that they name: Each block of 384 consecutive tokens has a mean vector of its own. `query_weight`: entries are those of a weight over 2048 inputs, of magnitude at most 6 / sqrt(2048). `key_weight`: entries are those of a weight over 2048 inputs, of magnitude at most 6 / sqrt(2048).
All inputs are finite; a program needn't handle non-finite values.
Results may differ from the reference program's by a relative error of at most 0.028.
Values may be sent and summed in bfloat16 or wider, within the bound.
A program may use at most 64 MiB of HBM per device.

```python
import math
import jax
import jax.numpy as jnp
from jax import lax

D = 2048
HEADS = 16
KV_HEADS = 4
HD = 64
GRID_W = 64
TOK_DEV = 384
TOKENS = 3072
N_TP = 4


def shared_query(key):
    base = jnp.clip(jax.random.normal(jax.random.fold_in(key, 11), (D, HEADS * HD), jnp.float32), -6.0, 6.0)
    base = base * D ** (-0.5)
    return base


def draw_tokens(key, part):
    offsets = jax.random.normal(jax.random.fold_in(key, 21), (TOKENS // TOK_DEV, D), jnp.float32)
    offsets = jnp.repeat(offsets, TOK_DEV, axis=0)
    noise = jax.random.normal(jax.random.fold_in(key, 22), (TOKENS, D), jnp.float32)
    return jnp.clip(noise + offsets, -8.0, 8.0).astype(jnp.bfloat16)


def draw_query_weight(key, part):
    return shared_query(key).astype(jnp.bfloat16)


def draw_key_weight(key, part):
    base = jnp.clip(jax.random.normal(jax.random.fold_in(key, 12), (D, KV_HEADS * HD), jnp.float32), -6.0, 6.0)
    return (base * D ** (-0.5)).astype(jnp.bfloat16)


def draw_query_gain(key, part):
    usual = jax.random.uniform(jax.random.fold_in(key, 31), (HEADS, HD), jnp.float32, 0.5, 1.5)
    return usual.astype(jnp.bfloat16)


def draw_key_gain(key, part):
    return jax.random.uniform(jax.random.fold_in(key, 41), (KV_HEADS, HD), jnp.float32, 0.5, 1.5).astype(jnp.bfloat16)


def level_of(key, shape, shards, low, largest):
    loudness = 1.0
    for dim, blocks in shards:
        draws = jax.random.uniform(jax.random.fold_in(jax.random.fold_in(key, 6), dim), (blocks,), jnp.float32, low / len(shards), largest / len(shards))
        loudness = loudness * jnp.repeat(jnp.exp(draws), shape[dim] // blocks).reshape((-1,) + (1,) * (len(shape) - 1 - dim))
    return loudness


def bell_draw(stream_key, dims, scale, reach, shards=(), held_as=jnp.bfloat16):
    loudness = level_of(stream_key, dims, shards, -0.22, 0.18) if shards else 1.0
    drawn = jax.random.normal(stream_key, dims, jnp.float32) * scale * loudness
    return jnp.minimum(jnp.maximum(drawn, -reach), reach).astype(held_as)


def setup_inputs(seed: int = 0) -> dict:
    key_of = jax.random.split(jax.random.key(seed), 8)
    return {
        "tokens": draw_tokens(jax.random.fold_in(key_of[7], 71), 0),
        "query_weight": draw_query_weight(jax.random.fold_in(key_of[7], 71), 0),
        "key_weight": draw_key_weight(jax.random.fold_in(key_of[7], 71), 0),
        "value_weight": bell_draw(key_of[3], (D, KV_HEADS * HD), D ** -0.5, 0.125, ((1, 4),)),
        "out_weight": bell_draw(key_of[4], (HEADS * HD, D), (HEADS * HD // 16) ** -0.5, 0.75, ((0, 4),)),
        "query_gain": draw_query_gain(jax.random.fold_in(key_of[7], 71), 0),
        "key_gain": draw_key_gain(jax.random.fold_in(key_of[7], 71), 0),
    }


def angle_tables(count):
    quarter = HD // 4
    place = jnp.arange(count, dtype=jnp.int32)
    grid_row = (place // GRID_W).astype(jnp.float32)
    grid_col = (place % GRID_W).astype(jnp.float32)
    freq = 10000.0 ** (-jnp.arange(quarter, dtype=jnp.float32).astype(jnp.float32) / quarter)
    row_angle = grid_row[:, None] * freq[None, :]
    col_angle = grid_col[:, None] * freq[None, :]
    return (jnp.cos(row_angle), jnp.sin(row_angle), jnp.cos(col_angle), jnp.sin(col_angle))

def turn_pairs(part, cosine, sine):
    quarter = part.shape[-1] // 2
    first = part[..., :quarter]
    second = part[..., quarter:]
    cosine = cosine[:, None, :]
    sine = sine[:, None, :]
    return jnp.concatenate([first * cosine - second * sine, second * cosine + first * sine], axis=-1)

def prepare(raw, gain, tables):
    count = raw.shape[0]
    heads = gain.shape[0]
    values = raw.astype(jnp.float32).reshape(count, heads, HD)
    scaled = values * lax.rsqrt(lax.optimization_barrier(jnp.mean(values * values, axis=-1, keepdims=True)) + 1e-06)
    scaled = scaled * gain.astype(jnp.float32)[None, :, :]
    half = HD // 2
    row_cos, row_sin, col_cos, col_sin = tables
    turned = jnp.concatenate([turn_pairs(scaled[..., :half], row_cos, row_sin), turn_pairs(scaled[..., half:], col_cos, col_sin)], axis=-1)
    return turned.astype(jnp.bfloat16)

def reference(tokens, query_weight, key_weight, value_weight, out_weight, query_gain, key_gain):
    count = tokens.shape[0]
    query_raw = jnp.dot(tokens, query_weight, preferred_element_type=jnp.float32).astype(jnp.bfloat16)
    key_raw = jnp.dot(tokens, key_weight, preferred_element_type=jnp.float32).astype(jnp.bfloat16)
    values = jnp.dot(tokens, value_weight, preferred_element_type=jnp.float32).astype(jnp.bfloat16)
    tables = angle_tables(count)
    queries = prepare(query_raw, query_gain, tables)
    keys = prepare(key_raw, key_gain, tables)
    share = HEADS // KV_HEADS
    key_float = keys.astype(jnp.float32)
    value_float = values.reshape(count, KV_HEADS, HD).astype(jnp.float32)
    block_len = math.gcd(count, 128)
    blocks = queries.reshape(count // block_len, block_len, KV_HEADS, share, HD)

    def one_block(query_block):
        scores = jnp.einsum('qhgd,khd->hgqk', query_block.astype(jnp.float32), key_float, precision=lax.Precision.HIGHEST) * HD ** (-0.5)
        row_max = lax.optimization_barrier(jnp.max(scores, axis=-1))
        expo = jnp.exp(scores - row_max[..., None])
        totals = lax.optimization_barrier(jnp.sum(expo, axis=-1))
        weights = lax.optimization_barrier(expo.astype(jnp.bfloat16)).astype(jnp.float32)
        summed = jnp.einsum('hgqk,khd->qhgd', weights, value_float, precision=lax.Precision.HIGHEST)
        attended = summed / jnp.transpose(totals, (2, 0, 1))[..., None]
        log_block = (row_max + jnp.log(totals)).reshape(HEADS, block_len)
        return (attended.astype(jnp.bfloat16).reshape(block_len, HEADS * HD), log_block)
    attended, log_blocks = lax.map(one_block, blocks)
    attended = attended.reshape(count, HEADS * HD)
    log_sums = jnp.transpose(log_blocks, (1, 0, 2)).reshape(HEADS, count)
    group_width = HEADS // N_TP * HD
    total = jnp.zeros((count, D), jnp.float32)
    for group in range(N_TP):
        lo = group * group_width
        partial_sum = jnp.dot(attended[:, lo:lo + group_width], out_weight[lo:lo + group_width], preferred_element_type=jnp.float32).astype(jnp.bfloat16)
        total = total + partial_sum.astype(jnp.float32)
    return (total.astype(jnp.bfloat16), log_sums)
```

```python
import functools
import math

import jax
import jax.numpy as jnp
from jax import lax
from jax.experimental import pallas as pl
from jax.experimental.pallas import tpu as pltpu
from jax.sharding import PartitionSpec as P

GRID_W = 64
ROPE_BASE = 10000.0
EPS = 1e-06
LOG2E = math.log2(math.e)
LN2 = math.log(2.0)
ONES = 16
MESH = pl.DeviceIdType.MESH
F32 = jnp.float32
BF16 = jnp.bfloat16


def prepare(x, gain, tables):
    quarter = x.shape[0] // 4
    x = x * lax.rsqrt(jnp.mean(x * x, axis=0, keepdims=True) + EPS) * gain
    a, b, c, d = (x[i * quarter : (i + 1) * quarter] for i in range(4))
    row_cos, row_sin, col_cos, col_sin = tables
    return jnp.concatenate(
        [
            a * row_cos - b * row_sin,
            b * row_cos + a * row_sin,
            c * col_cos - d * col_sin,
            d * col_cos + c * col_sin,
        ],
        axis=0,
    )


def angle_tables(first, count, quarter):
    place = first + lax.broadcasted_iota(jnp.int32, (quarter, count), 1)
    order = lax.broadcasted_iota(jnp.int32, (quarter, count), 0).astype(F32)
    freq = jnp.exp(order * (-math.log(ROPE_BASE) / quarter))
    shift = GRID_W.bit_length() - 1
    row = lax.shift_right_logical(place, shift).astype(F32) * freq
    col = jnp.bitwise_and(place, GRID_W - 1).astype(F32) * freq
    return (jnp.cos(row), jnp.sin(row), jnp.cos(col), jnp.sin(col))


def kernel(
    n_sp,
    n_tp,
    chunks,
    tok_hbm,
    wq_hbm,
    wk_hbm,
    wv_hbm,
    wo_hbm,
    qg_ref,
    kg_ref,
    mixed_ref,
    log_ref,
    tok,
    wq,
    wk,
    wv,
    wkv,
    wo,
    gains,
    raw,
    queries,
    kv,
    top,
    acc,
    att_own,
    att_out,
    att_in,
    part_out,
    part_in,
    local_sem,
    tok_send,
    tok_recv,
    wo_send,
    wo_recv,
    kv_send,
    kv_recv,
    att_send,
    att_recv,
    part_send,
    part_recv,
):
    sp = lax.axis_index("sp")
    tp = lax.axis_index("tp")
    pairs = n_tp // 2
    cols = n_sp // 2
    pair, core = tp // 2, tp % 2
    mate = pair * 2 + (1 - core)
    col, side = sp // 2, sp % 2
    other = col * 2 + (1 - side)
    rows = tok.shape[1]
    heads, width = qg_ref.shape
    kv_heads = kg_ref.shape[0]
    share = heads // kv_heads
    count = rows * n_tp

    def across(i):
        return lax.rem(pair + i, pairs) * 2 + core

    def column(i):
        return lax.rem(col + i, cols) * 2 + side

    loads = [
        pltpu.make_async_copy(src, dst, local_sem.at[i])
        for i, (src, dst) in enumerate(
            ((tok_hbm, tok.at[tp]), (wq_hbm, wq), (wk_hbm, wk), (wv_hbm, wv), (wo_hbm, wo.at[core]))
        )
    ]
    for load in loads:
        load.start()

    barrier = pltpu.get_barrier_semaphore()
    peers = 0
    for i in range(1, pairs):
        pl.semaphore_signal(barrier, inc=1, device_id={"tp": across(i)}, device_id_type=MESH)
        peers += 1
    pl.semaphore_signal(barrier, inc=1, device_id={"tp": mate}, device_id_type=MESH)
    pl.semaphore_signal(barrier, inc=1, device_id={"sp": other}, device_id_type=MESH)
    peers += 2
    for i in range(1, cols):
        pl.semaphore_signal(barrier, inc=1, device_id={"sp": column(i)}, device_id_type=MESH)
        peers += 1
    pl.semaphore_wait(barrier, peers)

    def send(src, dst, send_sem, recv_sem, where):
        return pltpu.make_async_remote_copy(
            src_ref=src,
            dst_ref=dst,
            send_sem=send_sem,
            recv_sem=recv_sem,
            device_id=where,
            device_id_type=MESH,
        )

    pending = []

    def go(copy):
        copy.start()
        pending.append(copy)

    def token_copy(block, src, slot, target):
        return send(src, tok.at[block], tok_send.at[slot], tok_recv.at[block], {"tp": target})

    for i in range(1, pairs):
        go(token_copy(tp, tok_hbm, i, across(i)))
    go(token_copy(tp, tok_hbm, 0, mate))

    gains[...] = jnp.zeros_like(gains)
    gains[0:heads, 0:width] = qg_ref[...].astype(F32) * (LOG2E * width ** (-0.5))
    gains[heads : heads + kv_heads, 0:width] = kg_ref[...].astype(F32)
    turned_gains = jnp.transpose(gains[...])
    tables = angle_tables(sp * count, count, width // 4)
    top[...] = jnp.full_like(top, -1e30)
    acc[...] = jnp.zeros_like(acc)
    loads[2].wait()
    loads[3].wait()
    kv_cols = wk.shape[1]
    wkv[:, 0:kv_cols] = wk[...]
    wkv[:, kv_cols : 2 * kv_cols] = wv[...]
    loads[1].wait()
    loads[0].wait()
    query_cols = wq.shape[1]

    def project(block):
        piece = tok[block]
        at = pl.ds(pl.multiple_of(block * rows, rows), rows)
        raw[at, 0:query_cols] = jnp.dot(piece, wq[...], preferred_element_type=F32)
        raw[at, query_cols:] = jnp.dot(piece, wkv[...], preferred_element_type=F32)

    project(tp)
    token_copy(mate, tok_hbm, 0, mate).wait_recv()
    project(mate)
    for i in range(1, pairs):
        block = across(i)
        token_copy(block, tok_hbm, i, block).wait_recv()
        go(token_copy(block, tok.at[block], pairs + i, mate))
        project(block)
    loads[4].wait()
    wo_copy = send(wo_hbm, wo.at[core], wo_send, wo_recv, {"tp": mate})
    wo_copy.start()
    for i in range(1, pairs):
        block = lax.rem(pair + i, pairs) * 2 + (1 - core)
        token_copy(block, tok_hbm, i, mate).wait_recv()
        project(block)

    turned = jnp.transpose(raw[:, query_cols:])
    kv_rows = kv_heads * width
    for h in range(kv_heads):
        keys = prepare(
            turned[h * width : (h + 1) * width], turned_gains[0:width, heads + h : heads + h + 1], tables
        )
        kv[sp, h * width : (h + 1) * width, :] = keys.astype(BF16)
    kv[sp, kv_rows : 2 * kv_rows, :] = turned[kv_rows : 2 * kv_rows].astype(BF16)

    def kv_copy(block, slot, where):
        return send(kv.at[block], kv.at[block], kv_send.at[slot], kv_recv.at[block], {"sp": where})

    for i in range(1, cols):
        go(kv_copy(sp, i, column(i)))
    go(kv_copy(sp, 0, other))

    turned = jnp.transpose(raw[:, 0:query_cols])
    for h in range(heads):
        q = prepare(turned[h * width : (h + 1) * width], turned_gains[0:width, h : h + 1], tables)
        queries[h] = q.astype(BF16)

    def attend(block):
        ones = jnp.ones((ONES, count), BF16)
        for g in range(kv_heads):
            keys = jnp.transpose(kv[block, g * width : (g + 1) * width, :])
            values = kv[block, kv_rows + g * width : kv_rows + (g + 1) * width, :]
            values = jnp.concatenate([values, ones], axis=0)
            for h in range(g * share, (g + 1) * share):
                scores = jnp.dot(keys, queries[h], preferred_element_type=F32)
                old = top[h : h + 1, :]
                new = jnp.maximum(old, jnp.max(scores, axis=0, keepdims=True))
                weights = jnp.exp2(scores - new).astype(BF16)
                mixed = jnp.dot(values, weights, preferred_element_type=F32)
                acc[h] = acc[h] * jnp.exp2(old - new) + mixed
                top[h : h + 1, :] = new

    attend(sp)

    def step(i, carry):
        block = column(i)
        kv_copy(block, 0, block).wait_recv()
        kv_copy(block, cols + i, other).start()
        attend(block)
        late = lax.rem(col + i - 1, cols) * 2 + (1 - side)
        kv_copy(late, 0, other).wait_recv()
        attend(late)
        return carry

    lax.fori_loop(1, cols, step, 0)
    late = lax.rem(col + cols - 1, cols) * 2 + (1 - side)
    kv_copy(late, 0, other).wait_recv()
    attend(late)

    finished = []
    for h in range(heads):
        total = acc[h, width : width + 1, :]
        finished.append(acc[h, 0:width, :] / total)
        log_ref[h : h + 1, :] = (top[h : h + 1, :] + jnp.log2(total)) * LN2
    attended = jnp.transpose(jnp.concatenate(finished, axis=0)).astype(BF16)
    for t in range(n_tp):
        piece = attended[t * rows : (t + 1) * rows]

        @pl.when(core == t % 2)
        def _():
            att_own[t // 2] = piece

        @pl.when(core != t % 2)
        def _():
            att_out[t // 2] = piece

    att_copy = send(att_out, att_in, att_send, att_recv, {"tp": mate})
    att_copy.start()
    att_copy.wait_recv()
    wo_copy.wait_recv()
    step_cols = mixed_ref.shape[1] // chunks

    def product(place, n):
        at = slice(n * step_cols, (n + 1) * step_cols)
        return jnp.dot(
            att_own[place], wo[core, :, at], preferred_element_type=F32
        ) + jnp.dot(att_in[place], wo[1 - core, :, at], preferred_element_type=F32)

    def part_copy(i, n):
        slot = (i - 1) * chunks + n
        return send(
            part_out.at[slot],
            part_in.at[slot],
            part_send.at[slot],
            part_recv.at[slot],
            {"tp": across(i)},
        )

    for n in range(chunks):
        for i in range(1, pairs):
            part_out[(i - 1) * chunks + n] = product(lax.rem(pair + i, pairs), n).astype(BF16)
            part_copy(i, n).start()
    for n in range(chunks):
        at = slice(n * step_cols, (n + 1) * step_cols)
        total = product(pair, n)
        for i in range(1, pairs):
            part_copy(i, n).wait_recv()
            total = total + part_in[(i - 1) * chunks + n].astype(F32)
        mixed_ref[:, at] = total.astype(BF16)

    for copy in pending:
        copy.wait_send()
    wo_copy.wait_send()
    att_copy.wait_send()
    for i in range(1, cols):
        kv_copy(column(i), cols + i, other).wait_send()
    for n in range(chunks):
        for i in range(1, pairs):
            part_copy(i, n).wait_send()


def body(n_sp, n_tp, tokens, query_weight, key_weight, value_weight, out_weight, query_gain, key_gain):
    rows, depth = tokens.shape
    query_cols = query_weight.shape[1]
    kv_cols = key_weight.shape[1]
    heads, width = query_gain.shape
    kv_heads = key_gain.shape[0]
    group, model = out_weight.shape
    count = rows * n_tp
    pairs, cols = n_tp // 2, n_sp // 2
    chunks = 4
    any_space = pl.BlockSpec(memory_space=pl.ANY)
    vmem = pl.BlockSpec(memory_space=pltpu.VMEM)
    dma = pltpu.SemaphoreType.DMA
    slots = max(pairs - 1, 1) * chunks
    return pl.pallas_call(
        functools.partial(kernel, n_sp, n_tp, chunks),
        out_shape=(
            jax.ShapeDtypeStruct((rows, model), BF16),
            jax.ShapeDtypeStruct((heads, count), F32),
        ),
        in_specs=[any_space] * 5 + [vmem] * 2,
        out_specs=(vmem, vmem),
        scratch_shapes=[
            pltpu.VMEM((n_tp, rows, depth), BF16),
            pltpu.VMEM((depth, query_cols), BF16),
            pltpu.VMEM((depth, kv_cols), BF16),
            pltpu.VMEM((depth, kv_cols), BF16),
            pltpu.VMEM((depth, 2 * kv_cols), BF16),
            pltpu.VMEM((2, group, model), BF16),
            pltpu.VMEM((128, 128), F32),
            pltpu.VMEM((count, query_cols + 2 * kv_cols), F32),
            pltpu.VMEM((heads, width, count), BF16),
            pltpu.VMEM((n_sp, 2 * kv_heads * width, count), BF16),
            pltpu.VMEM((heads, count), F32),
            pltpu.VMEM((heads, width + ONES, count), F32),
            pltpu.VMEM((pairs, rows, group), BF16),
            pltpu.VMEM((pairs, rows, group), BF16),
            pltpu.VMEM((pairs, rows, group), BF16),
            pltpu.VMEM((slots, rows, model // chunks), BF16),
            pltpu.VMEM((slots, rows, model // chunks), BF16),
            dma((5,)),
            dma((2 * pairs,)),
            dma((n_tp,)),
            dma,
            dma,
            dma((2 * cols,)),
            dma((n_sp,)),
            dma,
            dma,
            dma((slots,)),
            dma((slots,)),
        ],
        compiler_params=pltpu.CompilerParams(
            collective_id=0, has_side_effects=True, vmem_limit_bytes=60 * 1024 * 1024
        ),
        name="attention",
    )(tokens, query_weight, key_weight, value_weight, out_weight, query_gain, key_gain)


def solution(mesh):
    return jax.shard_map(
        functools.partial(body, mesh.shape["sp"], mesh.shape["tp"]),
        mesh=mesh,
        in_specs=(
            P(("sp", "tp"), None),
            P(None, "tp"),
            P(None, "tp"),
            P(None, "tp"),
            P("tp", None),
            P("tp", None),
            P("tp", None),
        ),
        out_specs=(P(("sp", "tp"), None), P("tp", "sp")),
        check_vma=False,
    )
```

```python
import functools
import math

import jax
import jax.numpy as jnp
from jax import lax
from jax.experimental import pallas as pl
from jax.experimental.pallas import tpu as pltpu
from jax.sharding import PartitionSpec as P

GRID_W = 64
ROPE_BASE = 10000.0
EPS = 1e-06
LOG2E = math.log2(math.e)
LN2 = math.log(2.0)
ONES = 16
MESH = pl.DeviceIdType.MESH
F32 = jnp.float32
BF16 = jnp.bfloat16


def prepare(x, gain, tables):
    quarter = x.shape[0] // 4
    x = x * lax.rsqrt(jnp.mean(x * x, axis=0, keepdims=True) + EPS) * gain
    a, b, c, d = (x[i * quarter : (i + 1) * quarter] for i in range(4))
    row_cos, row_sin, col_cos, col_sin = tables
    return jnp.concatenate(
        [
            a * row_cos - b * row_sin,
            b * row_cos + a * row_sin,
            c * col_cos - d * col_sin,
            d * col_cos + c * col_sin,
        ],
        axis=0,
    )


def angle_tables(first, count, quarter):
    place = first + lax.broadcasted_iota(jnp.int32, (quarter, count), 1)
    order = lax.broadcasted_iota(jnp.int32, (quarter, count), 0).astype(F32)
    freq = jnp.exp(order * (-math.log(ROPE_BASE) / quarter))
    shift = GRID_W.bit_length() - 1
    row = lax.shift_right_logical(place, shift).astype(F32) * freq
    col = jnp.bitwise_and(place, GRID_W - 1).astype(F32) * freq
    return (jnp.cos(row), jnp.sin(row), jnp.cos(col), jnp.sin(col))


def kernel(
    n_sp,
    n_tp,
    chunks,
    tok_hbm,
    wq_hbm,
    wk_hbm,
    wv_hbm,
    wo_hbm,
    qg_ref,
    kg_ref,
    mixed_ref,
    log_ref,
    tok,
    wq,
    wkv,
    wo,
    gains,
    raw,
    queries,
    kv,
    top,
    acc,
    att_own,
    att_out,
    att_in,
    part_out,
    part_in,
    local_sem,
    tok_send,
    tok_recv,
    wo_send,
    wo_recv,
    kv_send,
    kv_recv,
    att_send,
    att_recv,
    part_send,
    part_recv,
):
    sp = lax.axis_index("sp")
    tp = lax.axis_index("tp")
    pairs = n_tp // 2
    cols = n_sp // 2
    pair, core = tp // 2, tp % 2
    mate = pair * 2 + (1 - core)
    col, side = sp // 2, sp % 2
    other = col * 2 + (1 - side)
    rows = tok.shape[1]
    heads, width = qg_ref.shape
    kv_heads = kg_ref.shape[0]
    share = heads // kv_heads
    count = rows * n_tp

    def across(i):
        return lax.rem(pair + i, pairs) * 2 + core

    kv_cols = wk_hbm.shape[0]
    loads = [
        pltpu.make_async_copy(src, dst, local_sem.at[i])
        for i, (src, dst) in enumerate(
            ((tok_hbm, tok.at[tp]), (wq_hbm, wq), (wk_hbm, wkv.at[0:kv_cols]), (wv_hbm, wkv.at[kv_cols:]), (wo_hbm, wo.at[core]))
        )
    ]
    for load in loads:
        load.start()

    barrier = pltpu.get_barrier_semaphore()
    peers = 0
    for i in range(1, pairs):
        pl.semaphore_signal(barrier, inc=1, device_id={"tp": across(i)}, device_id_type=MESH)
        peers += 1
    pl.semaphore_signal(barrier, inc=1, device_id={"tp": mate}, device_id_type=MESH)
    pl.semaphore_signal(barrier, inc=1, device_id={"sp": other}, device_id_type=MESH)
    peers += 2
    for way in (1, -1):
        near = lax.rem(col + way + cols, cols) * 2 + side
        pl.semaphore_signal(barrier, inc=1, device_id={"sp": near}, device_id_type=MESH)
        peers += 1
    pl.semaphore_wait(barrier, peers)

    def send(src, dst, send_sem, recv_sem, where):
        return pltpu.make_async_remote_copy(
            src_ref=src,
            dst_ref=dst,
            send_sem=send_sem,
            recv_sem=recv_sem,
            device_id=where,
            device_id_type=MESH,
        )

    pending = []

    def go(copy):
        copy.start()
        pending.append(copy)

    def token_copy(block, src, slot, target):
        return send(src, tok.at[block], tok_send.at[slot], tok_recv.at[block], {"tp": target})

    for i in range(1, pairs):
        go(token_copy(tp, tok_hbm, i, across(i)))
    go(token_copy(tp, tok_hbm, 0, mate))

    gains[...] = jnp.zeros_like(gains)
    gains[0:heads, 0:width] = qg_ref[...].astype(F32) * (LOG2E * width ** (-0.5))
    gains[heads : heads + kv_heads, 0:width] = kg_ref[...].astype(F32)
    turned_gains = jnp.transpose(gains[...])
    tables = angle_tables(sp * count, count, width // 4)
    top[...] = jnp.full_like(top, -1e30)
    acc[...] = jnp.zeros_like(acc)
    loads[2].wait()
    loads[3].wait()
    loads[1].wait()
    loads[0].wait()
    query_cols = wq.shape[1]

    def project(block):
        piece = tok[block]
        at = pl.ds(pl.multiple_of(block * rows, rows), rows)
        raw[at, 0:query_cols] = jnp.dot(piece, wq[...], preferred_element_type=F32)
        raw[at, query_cols:] = lax.dot_general(
            piece, wkv[...], (((1,), (1,)), ((), ())), preferred_element_type=F32
        )

    project(tp)
    token_copy(mate, tok_hbm, 0, mate).wait_recv()
    project(mate)
    for i in range(1, pairs):
        block = across(i)
        token_copy(block, tok_hbm, i, block).wait_recv()
        go(token_copy(block, tok.at[block], pairs + i, mate))
        project(block)
    loads[4].wait()
    wo_copy = send(wo_hbm, wo.at[core], wo_send, wo_recv, {"tp": mate})
    wo_copy.start()
    for i in range(1, pairs):
        block = lax.rem(pair + i, pairs) * 2 + (1 - core)
        token_copy(block, tok_hbm, i, mate).wait_recv()
        project(block)

    turned = jnp.transpose(raw[:, query_cols:])
    kv_rows = kv_heads * width
    for h in range(kv_heads):
        keys = prepare(
            turned[h * width : (h + 1) * width], turned_gains[0:width, heads + h : heads + h + 1], tables
        )
        kv[sp, h * width : (h + 1) * width, :] = keys.astype(BF16)
    kv[sp, kv_rows : 2 * kv_rows, :] = turned[kv_rows : 2 * kv_rows].astype(BF16)

    half = cols // 2
    mirror = 1 - side

    def column(i):
        return lax.rem(col + i + cols, cols)

    def kv_copy(block, part, slot, where):
        spot = kv.at[block]
        if part is not None:
            spot = kv.at[block, part * kv_rows : (part + 1) * kv_rows]
        return send(spot, spot, kv_send.at[slot], kv_recv.at[block, part or 0], {"sp": where})

    slots = iter(range(4 * n_sp))

    def pass_on(distance, s, way):
        if distance > half or (distance == half and s is mirror):
            return
        part = None if distance < half else (0 if way > 0 else 1)
        block = column(-(distance - 1) * way) * 2 + s
        go(kv_copy(block, part, next(slots), column(way) * 2 + side))

    def landed(distance, s, way):
        block = column(-distance * way) * 2 + s
        part = None if distance < half else (0 if way > 0 else 1)
        kv_copy(block, part, 0, other).wait_recv()
        return block

    go(kv_copy(sp, None, next(slots), other))
    for way in (1, -1):
        pass_on(1, side, way)

    turned = jnp.transpose(raw[:, 0:query_cols])
    for h in range(heads):
        q = prepare(turned[h * width : (h + 1) * width], turned_gains[0:width, h : h + 1], tables)
        queries[h] = q.astype(BF16)

    def attend(block):
        ones = jnp.ones((ONES, count), BF16)
        for g in range(kv_heads):
            keys = jnp.transpose(kv[block, g * width : (g + 1) * width, :])
            values = kv[block, kv_rows + g * width : kv_rows + (g + 1) * width, :]
            values = jnp.concatenate([values, ones], axis=0)
            for h in range(g * share, (g + 1) * share):
                scores = jnp.dot(keys, queries[h], preferred_element_type=F32)
                old = top[h : h + 1, :]
                new = jnp.maximum(old, jnp.max(scores, axis=0, keepdims=True))
                weights = jnp.exp2(scores - new).astype(BF16)
                mixed = jnp.dot(values, weights, preferred_element_type=F32)
                acc[h] = acc[h] * jnp.exp2(old - new) + mixed
                top[h : h + 1, :] = new

    attend(sp)
    kv_copy(other, None, 0, other).wait_recv()
    for way in (1, -1):
        pass_on(1, mirror, way)
    attend(other)

    def opposite():
        for way in (1, -1):
            block = landed(half, side, way)
        go(kv_copy(block, None, next(slots), other))
        return block

    for distance in range(1, half):
        arrived = []
        for way in (1, -1):
            arrived.append(landed(distance, side, way))
            pass_on(distance + 1, side, way)
        for block in arrived:
            attend(block)
        if distance == half - 1:
            last = opposite()
        arrived = []
        for way in (1, -1):
            arrived.append(landed(distance, mirror, way))
            pass_on(distance + 1, mirror, way)
        for block in arrived:
            attend(block)
    if half == 1:
        last = opposite()
    attend(last)
    last = column(half) * 2 + mirror
    kv_copy(last, None, 0, other).wait_recv()
    attend(last)

    finished = []
    for h in range(heads):
        total = acc[h, width : width + 1, :]
        finished.append(acc[h, 0:width, :] / total)
        log_ref[h : h + 1, :] = (top[h : h + 1, :] + jnp.log2(total)) * LN2
    attended = jnp.transpose(jnp.concatenate(finished, axis=0)).astype(BF16)
    for t in range(n_tp):
        piece = attended[t * rows : (t + 1) * rows]

        @pl.when(core == t % 2)
        def _():
            att_own[t // 2] = piece

        @pl.when(core != t % 2)
        def _():
            att_out[t // 2] = piece

    att_copy = send(att_out, att_in, att_send, att_recv, {"tp": mate})
    att_copy.start()
    att_copy.wait_recv()
    wo_copy.wait_recv()
    step_cols = mixed_ref.shape[1] // chunks

    def product(place, n):
        at = slice(n * step_cols, (n + 1) * step_cols)
        return jnp.dot(
            att_own[place], wo[core, :, at], preferred_element_type=F32
        ) + jnp.dot(att_in[place], wo[1 - core, :, at], preferred_element_type=F32)

    def part_copy(i, n):
        slot = (i - 1) * chunks + n
        return send(
            part_out.at[slot],
            part_in.at[slot],
            part_send.at[slot],
            part_recv.at[slot],
            {"tp": across(i)},
        )

    for n in range(chunks):
        for i in range(1, pairs):
            part_out[(i - 1) * chunks + n] = product(lax.rem(pair + i, pairs), n).astype(BF16)
            part_copy(i, n).start()
    for n in range(chunks):
        at = slice(n * step_cols, (n + 1) * step_cols)
        total = product(pair, n)
        for i in range(1, pairs):
            part_copy(i, n).wait_recv()
            total = total + part_in[(i - 1) * chunks + n].astype(F32)
        mixed_ref[:, at] = total.astype(BF16)

    for copy in pending:
        copy.wait_send()
    wo_copy.wait_send()
    att_copy.wait_send()
    for n in range(chunks):
        for i in range(1, pairs):
            part_copy(i, n).wait_send()


def body(n_sp, n_tp, tokens, query_weight, key_weight, value_weight, out_weight, query_gain, key_gain):
    rows, depth = tokens.shape
    query_cols = query_weight.shape[1]
    kv_cols = key_weight.shape[1]
    heads, width = query_gain.shape
    kv_heads = key_gain.shape[0]
    group, model = out_weight.shape
    count = rows * n_tp
    pairs = n_tp // 2
    chunks = 4
    any_space = pl.BlockSpec(memory_space=pl.ANY)
    vmem = pl.BlockSpec(memory_space=pltpu.VMEM)
    dma = pltpu.SemaphoreType.DMA
    slots = max(pairs - 1, 1) * chunks
    return pl.pallas_call(
        functools.partial(kernel, n_sp, n_tp, chunks),
        out_shape=(
            pltpu.VMEM((rows, model), BF16),
            pltpu.VMEM((heads, count), F32),
        ),
        in_specs=[any_space] * 5 + [vmem] * 2,
        out_specs=(vmem, vmem),
        scratch_shapes=[
            pltpu.VMEM((n_tp, rows, depth), BF16),
            pltpu.VMEM((depth, query_cols), BF16),
            pltpu.VMEM((2 * kv_cols, depth), BF16),
            pltpu.VMEM((2, group, model), BF16),
            pltpu.VMEM((128, 128), F32),
            pltpu.VMEM((count, query_cols + 2 * kv_cols), F32),
            pltpu.VMEM((heads, width, count), BF16),
            pltpu.VMEM((n_sp, 2 * kv_heads * width, count), BF16),
            pltpu.VMEM((heads, count), F32),
            pltpu.VMEM((heads, width + ONES, count), F32),
            pltpu.VMEM((pairs, rows, group), BF16),
            pltpu.VMEM((pairs, rows, group), BF16),
            pltpu.VMEM((pairs, rows, group), BF16),
            pltpu.VMEM((slots, rows, model // chunks), BF16),
            pltpu.VMEM((slots, rows, model // chunks), BF16),
            dma((5,)),
            dma((2 * pairs,)),
            dma((n_tp,)),
            dma,
            dma,
            dma((4 * n_sp,)),
            dma((n_sp, 2)),
            dma,
            dma,
            dma((slots,)),
            dma((slots,)),
        ],
        compiler_params=pltpu.CompilerParams(
            collective_id=0, has_side_effects=True, vmem_limit_bytes=60 * 1024 * 1024
        ),
        name="attention",
    )(tokens, query_weight, key_weight.T, value_weight.T, out_weight, query_gain, key_gain)


def solution(mesh):
    return jax.shard_map(
        functools.partial(body, mesh.shape["sp"], mesh.shape["tp"]),
        mesh=mesh,
        in_specs=(
            P(("sp", "tp"), None),
            P(None, "tp"),
            P(None, "tp"),
            P(None, "tp"),
            P("tp", None),
            P("tp", None),
            P("tp", None),
        ),
        out_specs=(P(("sp", "tp"), None), P("tp", "sp")),
        check_vma=False,
    )
```

```python
import functools
import math

import jax
import jax.numpy as jnp
from jax import lax
from jax.experimental import pallas as pl
from jax.experimental.pallas import tpu as pltpu
from jax.sharding import PartitionSpec as P

GRID_W = 64
ROPE_BASE = 10000.0
EPS = 1e-06
LOG2E = math.log2(math.e)
LN2 = math.log(2.0)
ONES = 16
MESH = pl.DeviceIdType.MESH
F32 = jnp.float32
BF16 = jnp.bfloat16


def prepare(x, gain, tables):
    quarter = x.shape[0] // 4
    x = x * lax.rsqrt(jnp.mean(x * x, axis=0, keepdims=True) + EPS) * gain
    a, b, c, d = (x[i * quarter : (i + 1) * quarter] for i in range(4))
    row_cos, row_sin, col_cos, col_sin = tables
    return jnp.concatenate(
        [
            a * row_cos - b * row_sin,
            b * row_cos + a * row_sin,
            c * col_cos - d * col_sin,
            d * col_cos + c * col_sin,
        ],
        axis=0,
    )


def angle_tables(first, count, quarter):
    place = first + lax.broadcasted_iota(jnp.int32, (quarter, count), 1)
    order = lax.broadcasted_iota(jnp.int32, (quarter, count), 0).astype(F32)
    freq = jnp.exp(order * (-math.log(ROPE_BASE) / quarter))
    shift = GRID_W.bit_length() - 1
    row = lax.shift_right_logical(place, shift).astype(F32) * freq
    col = jnp.bitwise_and(place, GRID_W - 1).astype(F32) * freq
    return (jnp.cos(row), jnp.sin(row), jnp.cos(col), jnp.sin(col))


def kernel(
    n_sp,
    n_tp,
    chunks,
    tok_hbm,
    wq_hbm,
    wk_hbm,
    wv_hbm,
    wo_hbm,
    qg_ref,
    kg_ref,
    mixed_ref,
    log_ref,
    tok,
    wq,
    wkv,
    wo,
    gains,
    raw,
    queries,
    kv,
    top,
    acc,
    att_own,
    att_out,
    att_in,
    part_out,
    part_in,
    local_sem,
    tok_send,
    tok_recv,
    wo_send,
    wo_recv,
    kv_send,
    kv_recv,
    att_send,
    att_recv,
    part_send,
    part_recv,
):
    sp = lax.axis_index("sp")
    tp = lax.axis_index("tp")
    pairs = n_tp // 2
    cols = n_sp // 2
    pair, core = tp // 2, tp % 2
    mate = pair * 2 + (1 - core)
    col, side = sp // 2, sp % 2
    other = col * 2 + (1 - side)
    rows = tok.shape[1]
    heads, width = qg_ref.shape
    kv_heads = kg_ref.shape[0]
    share = heads // kv_heads
    count = rows * n_tp

    def across(i):
        return lax.rem(pair + i, pairs) * 2 + core

    kv_cols = wk_hbm.shape[0]
    loads = [
        pltpu.make_async_copy(src, dst, local_sem.at[i])
        for i, (src, dst) in enumerate(
            ((tok_hbm, tok.at[tp]), (wq_hbm, wq), (wk_hbm, wkv.at[0:kv_cols]), (wv_hbm, wkv.at[kv_cols:]), (wo_hbm, wo.at[core]))
        )
    ]
    for load in loads:
        load.start()

    barrier = pltpu.get_barrier_semaphore()
    peers = 0
    for i in range(1, pairs):
        pl.semaphore_signal(barrier, inc=1, device_id={"tp": across(i)}, device_id_type=MESH)
        peers += 1
    pl.semaphore_signal(barrier, inc=1, device_id={"tp": mate}, device_id_type=MESH)
    pl.semaphore_signal(barrier, inc=1, device_id={"sp": other}, device_id_type=MESH)
    peers += 2
    for i in range(1, cols):
        peer = lax.rem(col + i, cols) * 2 + side
        pl.semaphore_signal(barrier, inc=1, device_id={"sp": peer}, device_id_type=MESH)
        peers += 1
    pl.semaphore_wait(barrier, peers)

    def send(src, dst, send_sem, recv_sem, where):
        return pltpu.make_async_remote_copy(
            src_ref=src,
            dst_ref=dst,
            send_sem=send_sem,
            recv_sem=recv_sem,
            device_id=where,
            device_id_type=MESH,
        )

    pending = []

    def go(copy):
        copy.start()
        pending.append(copy)

    def token_copy(block, src, slot, target):
        return send(src, tok.at[block], tok_send.at[slot], tok_recv.at[block], {"tp": target})

    for i in range(1, pairs):
        go(token_copy(tp, tok_hbm, i, across(i)))
    go(token_copy(tp, tok_hbm, 0, mate))

    gains[...] = jnp.zeros_like(gains)
    gains[0:heads, 0:width] = qg_ref[...].astype(F32) * (LOG2E * width ** (-0.5))
    gains[heads : heads + kv_heads, 0:width] = kg_ref[...].astype(F32)
    turned_gains = jnp.transpose(gains[...])
    tables = angle_tables(sp * count, count, width // 4)
    top[...] = jnp.full_like(top, -1e30)
    acc[...] = jnp.zeros_like(acc)
    loads[2].wait()
    loads[3].wait()
    loads[1].wait()
    loads[0].wait()
    query_cols = wq.shape[1]

    def project(block):
        piece = tok[block]
        at = pl.ds(pl.multiple_of(block * rows, rows), rows)
        raw[at, 0:query_cols] = jnp.dot(piece, wq[...], preferred_element_type=F32)
        raw[at, query_cols:] = lax.dot_general(
            piece, wkv[...], (((1,), (1,)), ((), ())), preferred_element_type=F32
        )

    project(tp)
    token_copy(mate, tok_hbm, 0, mate).wait_recv()
    project(mate)
    for i in range(1, pairs):
        block = across(i)
        token_copy(block, tok_hbm, i, block).wait_recv()
        go(token_copy(block, tok.at[block], pairs + i, mate))
        project(block)
    loads[4].wait()
    wo_copy = send(wo_hbm, wo.at[core], wo_send, wo_recv, {"tp": mate})
    wo_copy.start()
    for i in range(1, pairs):
        block = lax.rem(pair + i, pairs) * 2 + (1 - core)
        token_copy(block, tok_hbm, i, mate).wait_recv()
        project(block)

    turned = jnp.transpose(raw[:, query_cols:])
    kv_rows = kv_heads * width
    for h in range(kv_heads):
        keys = prepare(
            turned[h * width : (h + 1) * width], turned_gains[0:width, heads + h : heads + h + 1], tables
        )
        kv[sp, h * width : (h + 1) * width, :] = keys.astype(BF16)
    kv[sp, kv_rows : 2 * kv_rows, :] = turned[kv_rows : 2 * kv_rows].astype(BF16)

    def kv_copy(block, slot, where):
        return send(kv.at[block], kv.at[block], kv_send.at[slot], kv_recv.at[block], {"sp": where})

    def near(distance, act):
        for way in (1, -1):
            place = col + distance * way

            @pl.when(jnp.logical_and(place >= 0, place < cols))
            def _():
                act(place)

    def to_column(place):
        return kv_copy(sp, place, place * 2 + side)

    def to_other(place):
        return kv_copy(place * 2 + side, cols + place, other)

    to_other(col).start()
    for distance in range(1, cols):
        near(distance, lambda place: to_column(place).start())

    turned = jnp.transpose(raw[:, 0:query_cols])
    for h in range(heads):
        q = prepare(turned[h * width : (h + 1) * width], turned_gains[0:width, h : h + 1], tables)
        queries[h] = q.astype(BF16)

    def attend(block):
        ones = jnp.ones((ONES, count), BF16)
        for g in range(kv_heads):
            keys = jnp.transpose(kv[block, g * width : (g + 1) * width, :])
            values = kv[block, kv_rows + g * width : kv_rows + (g + 1) * width, :]
            values = jnp.concatenate([values, ones], axis=0)
            for h in range(g * share, (g + 1) * share):
                scores = jnp.dot(keys, queries[h], preferred_element_type=F32)
                old = top[h : h + 1, :]
                new = jnp.maximum(old, jnp.max(scores, axis=0, keepdims=True))
                weights = jnp.exp2(scores - new).astype(BF16)
                mixed = jnp.dot(values, weights, preferred_element_type=F32)
                acc[h] = acc[h] * jnp.exp2(old - new) + mixed
                top[h : h + 1, :] = new

    def straight(place):
        kv_copy(place * 2 + side, 0, other).wait_recv()
        to_other(place).start()
        attend(place * 2 + side)

    def mirrored(place):
        block = place * 2 + (1 - side)
        kv_copy(block, 0, other).wait_recv()
        attend(block)

    attend(sp)
    mirrored(col)

    def step(distance, carry):
        near(distance, straight)

        @pl.when(distance > 1)
        def _():
            near(distance - 1, mirrored)

        return carry

    lax.fori_loop(1, cols, step, 0)
    near(cols - 1, mirrored)

    finished = []
    for h in range(heads):
        total = acc[h, width : width + 1, :]
        finished.append(acc[h, 0:width, :] / total)
        log_ref[h : h + 1, :] = (top[h : h + 1, :] + jnp.log2(total)) * LN2
    attended = jnp.transpose(jnp.concatenate(finished, axis=0)).astype(BF16)
    for t in range(n_tp):
        piece = attended[t * rows : (t + 1) * rows]

        @pl.when(core == t % 2)
        def _():
            att_own[t // 2] = piece

        @pl.when(core != t % 2)
        def _():
            att_out[t // 2] = piece

    att_copy = send(att_out, att_in, att_send, att_recv, {"tp": mate})
    att_copy.start()
    att_copy.wait_recv()
    wo_copy.wait_recv()
    step_cols = mixed_ref.shape[1] // chunks

    def product(place, n):
        at = slice(n * step_cols, (n + 1) * step_cols)
        return jnp.dot(
            att_own[place], wo[core, :, at], preferred_element_type=F32
        ) + jnp.dot(att_in[place], wo[1 - core, :, at], preferred_element_type=F32)

    def part_copy(i, n):
        slot = (i - 1) * chunks + n
        return send(
            part_out.at[slot],
            part_in.at[slot],
            part_send.at[slot],
            part_recv.at[slot],
            {"tp": across(i)},
        )

    for n in range(chunks):
        for i in range(1, pairs):
            part_out[(i - 1) * chunks + n] = product(lax.rem(pair + i, pairs), n).astype(BF16)
            part_copy(i, n).start()
    for n in range(chunks):
        at = slice(n * step_cols, (n + 1) * step_cols)
        total = product(pair, n)
        for i in range(1, pairs):
            part_copy(i, n).wait_recv()
            total = total + part_in[(i - 1) * chunks + n].astype(F32)
        mixed_ref[:, at] = total.astype(BF16)

    for copy in pending:
        copy.wait_send()
    wo_copy.wait_send()
    att_copy.wait_send()
    to_other(col).wait_send()
    for distance in range(1, cols):
        near(distance, lambda place: to_column(place).wait_send())
        near(distance, lambda place: to_other(place).wait_send())
    for n in range(chunks):
        for i in range(1, pairs):
            part_copy(i, n).wait_send()


def body(n_sp, n_tp, tokens, query_weight, key_weight, value_weight, out_weight, query_gain, key_gain):
    rows, depth = tokens.shape
    query_cols = query_weight.shape[1]
    kv_cols = key_weight.shape[1]
    heads, width = query_gain.shape
    kv_heads = key_gain.shape[0]
    group, model = out_weight.shape
    count = rows * n_tp
    pairs, cols = n_tp // 2, n_sp // 2
    chunks = 4
    any_space = pl.BlockSpec(memory_space=pl.ANY)
    vmem = pl.BlockSpec(memory_space=pltpu.VMEM)
    dma = pltpu.SemaphoreType.DMA
    slots = max(pairs - 1, 1) * chunks
    return pl.pallas_call(
        functools.partial(kernel, n_sp, n_tp, chunks),
        out_shape=(
            pltpu.VMEM((rows, model), BF16),
            pltpu.VMEM((heads, count), F32),
        ),
        in_specs=[any_space] * 5 + [vmem] * 2,
        out_specs=(vmem, vmem),
        scratch_shapes=[
            pltpu.VMEM((n_tp, rows, depth), BF16),
            pltpu.VMEM((depth, query_cols), BF16),
            pltpu.VMEM((2 * kv_cols, depth), BF16),
            pltpu.VMEM((2, group, model), BF16),
            pltpu.VMEM((128, 128), F32),
            pltpu.VMEM((count, query_cols + 2 * kv_cols), F32),
            pltpu.VMEM((heads, width, count), BF16),
            pltpu.VMEM((n_sp, 2 * kv_heads * width, count), BF16),
            pltpu.VMEM((heads, count), F32),
            pltpu.VMEM((heads, width + ONES, count), F32),
            pltpu.VMEM((pairs, rows, group), BF16),
            pltpu.VMEM((pairs, rows, group), BF16),
            pltpu.VMEM((pairs, rows, group), BF16),
            pltpu.VMEM((slots, rows, model // chunks), BF16),
            pltpu.VMEM((slots, rows, model // chunks), BF16),
            dma((5,)),
            dma((2 * pairs,)),
            dma((n_tp,)),
            dma,
            dma,
            dma((2 * cols,)),
            dma((n_sp,)),
            dma,
            dma,
            dma((slots,)),
            dma((slots,)),
        ],
        compiler_params=pltpu.CompilerParams(
            collective_id=0, has_side_effects=True, vmem_limit_bytes=60 * 1024 * 1024
        ),
        name="attention",
    )(tokens, query_weight, key_weight.T, value_weight.T, out_weight, query_gain, key_gain)


def solution(mesh):
    return jax.shard_map(
        functools.partial(body, mesh.shape["sp"], mesh.shape["tp"]),
        mesh=mesh,
        in_specs=(
            P(("sp", "tp"), None),
            P(None, "tp"),
            P(None, "tp"),
            P(None, "tp"),
            P("tp", None),
            P("tp", None),
            P("tp", None),
        ),
        out_specs=(P(("sp", "tp"), None), P("tp", "sp")),
        check_vma=False,
    )
```

```python
import functools
import math

import jax
import jax.numpy as jnp
from jax import lax
from jax.experimental import pallas as pl
from jax.experimental.pallas import tpu as pltpu
from jax.sharding import PartitionSpec as P

GRID_W = 64
ROPE_BASE = 10000.0
EPS = 1e-06
LOG2E = math.log2(math.e)
LN2 = math.log(2.0)
ONES = 16
MESH = pl.DeviceIdType.MESH
F32 = jnp.float32
BF16 = jnp.bfloat16


def prepare(x, gain, tables):
    quarter = x.shape[0] // 4
    x = x * lax.rsqrt(jnp.mean(x * x, axis=0, keepdims=True) + EPS) * gain
    a, b, c, d = (x[i * quarter : (i + 1) * quarter] for i in range(4))
    row_cos, row_sin, col_cos, col_sin = tables
    return jnp.concatenate(
        [
            a * row_cos - b * row_sin,
            b * row_cos + a * row_sin,
            c * col_cos - d * col_sin,
            d * col_cos + c * col_sin,
        ],
        axis=0,
    )


def angle_tables(first, count, quarter):
    place = first + lax.broadcasted_iota(jnp.int32, (quarter, count), 1)
    order = lax.broadcasted_iota(jnp.int32, (quarter, count), 0).astype(F32)
    freq = jnp.exp(order * (-math.log(ROPE_BASE) / quarter))
    shift = GRID_W.bit_length() - 1
    row = lax.shift_right_logical(place, shift).astype(F32) * freq
    col = jnp.bitwise_and(place, GRID_W - 1).astype(F32) * freq
    return (jnp.cos(row), jnp.sin(row), jnp.cos(col), jnp.sin(col))


def kernel(
    n_sp,
    n_tp,
    chunks,
    tok_hbm,
    wq_hbm,
    wk_hbm,
    wv_hbm,
    wo_hbm,
    qg_ref,
    kg_ref,
    mixed_ref,
    log_ref,
    tok,
    wq,
    wkv,
    wo,
    gains,
    raw,
    queries,
    kv,
    top,
    acc,
    att_own,
    att_out,
    att_in,
    part_out,
    part_in,
    local_sem,
    tok_send,
    tok_recv,
    wo_send,
    wo_recv,
    kv_send,
    kv_recv,
    att_send,
    att_recv,
    part_send,
    part_recv,
):
    sp = lax.axis_index("sp")
    tp = lax.axis_index("tp")
    pairs = n_tp // 2
    cols = n_sp // 2
    pair, core = tp // 2, tp % 2
    mate = pair * 2 + (1 - core)
    col, side = sp // 2, sp % 2
    other = col * 2 + (1 - side)
    rows = tok.shape[1]
    heads, width = qg_ref.shape
    kv_heads = kg_ref.shape[0]
    share = heads // kv_heads
    count = rows * n_tp

    def across(i):
        return lax.rem(pair + i, pairs) * 2 + core

    kv_cols = wk_hbm.shape[0]
    loads = [
        pltpu.make_async_copy(src, dst, local_sem.at[i])
        for i, (src, dst) in enumerate(
            ((tok_hbm, tok.at[tp]), (wq_hbm, wq), (wk_hbm, wkv.at[0:kv_cols]), (wv_hbm, wkv.at[kv_cols:]), (wo_hbm, wo.at[core]))
        )
    ]
    for load in loads:
        load.start()

    barrier = pltpu.get_barrier_semaphore()
    peers = 0
    for i in range(1, pairs):
        pl.semaphore_signal(barrier, inc=1, device_id={"tp": across(i)}, device_id_type=MESH)
        peers += 1
    pl.semaphore_signal(barrier, inc=1, device_id={"tp": mate}, device_id_type=MESH)
    pl.semaphore_signal(barrier, inc=1, device_id={"sp": other}, device_id_type=MESH)
    peers += 2
    for i in range(1, cols):
        peer = lax.rem(col + i, cols) * 2 + side
        pl.semaphore_signal(barrier, inc=1, device_id={"sp": peer}, device_id_type=MESH)
        peers += 1
    pl.semaphore_wait(barrier, peers)

    def send(src, dst, send_sem, recv_sem, where):
        return pltpu.make_async_remote_copy(
            src_ref=src,
            dst_ref=dst,
            send_sem=send_sem,
            recv_sem=recv_sem,
            device_id=where,
            device_id_type=MESH,
        )

    pending = []

    def go(copy):
        copy.start()
        pending.append(copy)

    def token_copy(block, src, slot, target):
        return send(src, tok.at[block], tok_send.at[slot], tok_recv.at[block], {"tp": target})

    for i in range(1, pairs):
        go(token_copy(tp, tok_hbm, i, across(i)))
    go(token_copy(tp, tok_hbm, 0, mate))

    gains[...] = jnp.zeros_like(gains)
    gains[0:heads, 0:width] = qg_ref[...].astype(F32) * (LOG2E * width ** (-0.5))
    gains[heads : heads + kv_heads, 0:width] = kg_ref[...].astype(F32)
    turned_gains = jnp.transpose(gains[...])
    tables = angle_tables(sp * count, count, width // 4)
    top[...] = jnp.full_like(top, -1e30)
    acc[...] = jnp.zeros_like(acc)
    loads[2].wait()
    loads[3].wait()
    loads[1].wait()
    loads[0].wait()
    query_cols = wq.shape[1]

    def project(block):
        piece = tok[block]
        at = pl.ds(pl.multiple_of(block * rows, rows), rows)
        raw[at, 0:query_cols] = jnp.dot(piece, wq[...], preferred_element_type=F32)
        raw[at, query_cols:] = lax.dot_general(
            piece, wkv[...], (((1,), (1,)), ((), ())), preferred_element_type=F32
        )

    kv_rows = kv_heads * width
    span = 2 * rows

    def span_of(part):
        return pl.ds(pl.multiple_of(part * span, span), span)

    def make_kv(part):
        at = span_of(part)
        turned = jnp.transpose(raw[at, query_cols : query_cols + kv_rows])
        angles = angle_tables(sp * count + part * span, span, width // 4)
        for h in range(kv_heads):
            gain = turned_gains[0:width, heads + h : heads + h + 1]
            keys = prepare(turned[h * width : (h + 1) * width], gain, angles)
            kv[sp, at, h * width : (h + 1) * width] = jnp.transpose(keys).astype(BF16)
        kv[sp, at, kv_rows : 2 * kv_rows] = raw[at, query_cols + kv_rows :].astype(BF16)

    def kv_copy(block, part, slot, where):
        spot = kv.at[block, span_of(part)]
        return send(spot, spot, kv_send.at[slot, part], kv_recv.at[block, part], {"sp": where})

    def near(distance, act):
        for way in (1, -1):
            place = col + distance * way

            @pl.when(jnp.logical_and(place >= 0, place < cols))
            def _():
                act(place)

    def to_column(place, part):
        return kv_copy(sp, part, place, place * 2 + side)

    def to_other(place, part):
        return kv_copy(place * 2 + side, part, cols + place, other)

    def send_kv(part):
        to_other(col, part).start()
        for distance in range(1, cols):
            near(distance, lambda place: to_column(place, part).start())

    def forward(place, part):
        kv_copy(place * 2 + side, part, 0, other).wait_recv()
        to_other(place, part).start()

    project(tp)
    token_copy(mate, tok_hbm, 0, mate).wait_recv()
    project(mate)
    make_kv(pair)
    send_kv(pair)
    for i in range(1, pairs):
        block = across(i)
        token_copy(block, tok_hbm, i, block).wait_recv()
        go(token_copy(block, tok.at[block], pairs + i, mate))
        project(block)
    loads[4].wait()
    wo_copy = send(wo_hbm, wo.at[core], wo_send, wo_recv, {"tp": mate})
    wo_copy.start()
    for i in range(1, pairs):
        block = lax.rem(pair + i, pairs) * 2 + (1 - core)
        token_copy(block, tok_hbm, i, mate).wait_recv()
        project(block)
        part = lax.rem(pair + i, pairs)
        make_kv(part)
        send_kv(part)
    for distance in range(1, cols):
        near(distance, lambda place: forward(place, pair))

    turned = jnp.transpose(raw[:, 0:query_cols])
    for h in range(heads):
        q = prepare(turned[h * width : (h + 1) * width], turned_gains[0:width, h : h + 1], tables)
        queries[h] = q.astype(BF16)

    def attend(block):
        ones = jnp.ones((ONES, count), BF16)
        turned = jnp.transpose(kv[block])
        for g in range(kv_heads):
            keys = kv[block, :, g * width : (g + 1) * width]
            values = turned[kv_rows + g * width : kv_rows + (g + 1) * width]
            values = jnp.concatenate([values, ones], axis=0)
            for h in range(g * share, (g + 1) * share):
                scores = jnp.dot(keys, queries[h], preferred_element_type=F32)
                old = top[h : h + 1, :]
                new = jnp.maximum(old, jnp.max(scores, axis=0, keepdims=True))
                weights = jnp.exp2(scores - new).astype(BF16)
                mixed = jnp.dot(values, weights, preferred_element_type=F32)
                acc[h] = acc[h] * jnp.exp2(old - new) + mixed
                top[h : h + 1, :] = new

    def straight(place):
        for i in range(1, pairs):
            forward(place, lax.rem(pair + i, pairs))
        attend(place * 2 + side)

    def mirrored(place):
        block = place * 2 + (1 - side)
        for part in range(pairs):
            kv_copy(block, part, 0, other).wait_recv()
        attend(block)

    attend(sp)
    mirrored(col)

    def step(distance, carry):
        near(distance, straight)

        @pl.when(distance > 1)
        def _():
            near(distance - 1, mirrored)

        return carry

    lax.fori_loop(1, cols, step, 0)
    near(cols - 1, mirrored)

    finished = []
    for h in range(heads):
        total = acc[h, width : width + 1, :]
        finished.append(acc[h, 0:width, :] / total)
        log_ref[h : h + 1, :] = (top[h : h + 1, :] + jnp.log2(total)) * LN2
    attended = jnp.transpose(jnp.concatenate(finished, axis=0)).astype(BF16)
    for t in range(n_tp):
        piece = attended[t * rows : (t + 1) * rows]

        @pl.when(core == t % 2)
        def _():
            att_own[t // 2] = piece

        @pl.when(core != t % 2)
        def _():
            att_out[t // 2] = piece

    att_copy = send(att_out, att_in, att_send, att_recv, {"tp": mate})
    att_copy.start()
    att_copy.wait_recv()
    wo_copy.wait_recv()
    step_cols = mixed_ref.shape[1] // chunks

    def product(place, n):
        at = slice(n * step_cols, (n + 1) * step_cols)
        return jnp.dot(
            att_own[place], wo[core, :, at], preferred_element_type=F32
        ) + jnp.dot(att_in[place], wo[1 - core, :, at], preferred_element_type=F32)

    def part_copy(i, n):
        slot = (i - 1) * chunks + n
        return send(
            part_out.at[slot],
            part_in.at[slot],
            part_send.at[slot],
            part_recv.at[slot],
            {"tp": across(i)},
        )

    for n in range(chunks):
        for i in range(1, pairs):
            part_out[(i - 1) * chunks + n] = product(lax.rem(pair + i, pairs), n).astype(BF16)
            part_copy(i, n).start()
    for n in range(chunks):
        at = slice(n * step_cols, (n + 1) * step_cols)
        total = product(pair, n)
        for i in range(1, pairs):
            part_copy(i, n).wait_recv()
            total = total + part_in[(i - 1) * chunks + n].astype(F32)
        mixed_ref[:, at] = total.astype(BF16)

    for copy in pending:
        copy.wait_send()
    wo_copy.wait_send()
    att_copy.wait_send()
    for part in range(pairs):
        to_other(col, part).wait_send()
        for distance in range(1, cols):
            near(distance, lambda place: to_column(place, part).wait_send())
            near(distance, lambda place: to_other(place, part).wait_send())
    for n in range(chunks):
        for i in range(1, pairs):
            part_copy(i, n).wait_send()


def body(n_sp, n_tp, tokens, query_weight, key_weight, value_weight, out_weight, query_gain, key_gain):
    rows, depth = tokens.shape
    query_cols = query_weight.shape[1]
    kv_cols = key_weight.shape[1]
    heads, width = query_gain.shape
    kv_heads = key_gain.shape[0]
    group, model = out_weight.shape
    count = rows * n_tp
    pairs, cols = n_tp // 2, n_sp // 2
    chunks = 4
    any_space = pl.BlockSpec(memory_space=pl.ANY)
    vmem = pl.BlockSpec(memory_space=pltpu.VMEM)
    dma = pltpu.SemaphoreType.DMA
    slots = max(pairs - 1, 1) * chunks
    return pl.pallas_call(
        functools.partial(kernel, n_sp, n_tp, chunks),
        out_shape=(
            pltpu.VMEM((rows, model), BF16),
            pltpu.VMEM((heads, count), F32),
        ),
        in_specs=[any_space] * 5 + [vmem] * 2,
        out_specs=(vmem, vmem),
        scratch_shapes=[
            pltpu.VMEM((n_tp, rows, depth), BF16),
            pltpu.VMEM((depth, query_cols), BF16),
            pltpu.VMEM((2 * kv_cols, depth), BF16),
            pltpu.VMEM((2, group, model), BF16),
            pltpu.VMEM((128, 128), F32),
            pltpu.VMEM((count, query_cols + 2 * kv_cols), F32),
            pltpu.VMEM((heads, width, count), BF16),
            pltpu.VMEM((n_sp, count, 2 * kv_heads * width), BF16),
            pltpu.VMEM((heads, count), F32),
            pltpu.VMEM((heads, width + ONES, count), F32),
            pltpu.VMEM((pairs, rows, group), BF16),
            pltpu.VMEM((pairs, rows, group), BF16),
            pltpu.VMEM((pairs, rows, group), BF16),
            pltpu.VMEM((slots, rows, model // chunks), BF16),
            pltpu.VMEM((slots, rows, model // chunks), BF16),
            dma((5,)),
            dma((2 * pairs,)),
            dma((n_tp,)),
            dma,
            dma,
            dma((2 * cols, pairs)),
            dma((n_sp, pairs)),
            dma,
            dma,
            dma((slots,)),
            dma((slots,)),
        ],
        compiler_params=pltpu.CompilerParams(
            collective_id=0, has_side_effects=True, vmem_limit_bytes=60 * 1024 * 1024
        ),
        name="attention",
    )(tokens, query_weight, key_weight.T, value_weight.T, out_weight, query_gain, key_gain)


def solution(mesh):
    return jax.shard_map(
        functools.partial(body, mesh.shape["sp"], mesh.shape["tp"]),
        mesh=mesh,
        in_specs=(
            P(("sp", "tp"), None),
            P(None, "tp"),
            P(None, "tp"),
            P(None, "tp"),
            P("tp", None),
            P("tp", None),
            P("tp", None),
        ),
        out_specs=(P(("sp", "tp"), None), P("tp", "sp")),
        check_vma=False,
    )
```

```python
import functools
import math

import jax
import jax.numpy as jnp
from jax import lax
from jax.experimental import pallas as pl
from jax.experimental.pallas import tpu as pltpu
from jax.sharding import PartitionSpec as P

GRID_W = 64
ROPE_BASE = 10000.0
EPS = 1e-06
LOG2E = math.log2(math.e)
LN2 = math.log(2.0)
ONES = 16
MESH = pl.DeviceIdType.MESH
F32 = jnp.float32
BF16 = jnp.bfloat16


def prepare(x, gain, tables):
    quarter = x.shape[0] // 4
    x = x * lax.rsqrt(jnp.mean(x * x, axis=0, keepdims=True) + EPS) * gain
    a, b, c, d = (x[i * quarter : (i + 1) * quarter] for i in range(4))
    row_cos, row_sin, col_cos, col_sin = tables
    return jnp.concatenate(
        [
            a * row_cos - b * row_sin,
            b * row_cos + a * row_sin,
            c * col_cos - d * col_sin,
            d * col_cos + c * col_sin,
        ],
        axis=0,
    )


def angle_tables(first, count, quarter):
    place = first + lax.broadcasted_iota(jnp.int32, (quarter, count), 1)
    order = lax.broadcasted_iota(jnp.int32, (quarter, count), 0).astype(F32)
    freq = jnp.exp(order * (-math.log(ROPE_BASE) / quarter))
    shift = GRID_W.bit_length() - 1
    row = lax.shift_right_logical(place, shift).astype(F32) * freq
    col = jnp.bitwise_and(place, GRID_W - 1).astype(F32) * freq
    return (jnp.cos(row), jnp.sin(row), jnp.cos(col), jnp.sin(col))


def kernel(
    n_sp,
    n_tp,
    chunks,
    tok_hbm,
    wq_hbm,
    wk_hbm,
    wv_hbm,
    wo_hbm,
    qg_ref,
    kg_ref,
    mixed_ref,
    log_ref,
    tok,
    wq,
    wkv,
    wo,
    gains,
    raw,
    queries,
    kv,
    top,
    acc,
    att_own,
    att_out,
    att_in,
    part_out,
    part_in,
    local_sem,
    tok_send,
    tok_recv,
    wo_send,
    wo_recv,
    kv_send,
    kv_recv,
    att_send,
    att_recv,
    part_send,
    part_recv,
):
    sp = lax.axis_index("sp")
    tp = lax.axis_index("tp")
    pairs = n_tp // 2
    cols = n_sp // 2
    pair, core = tp // 2, tp % 2
    mate = pair * 2 + (1 - core)
    col, side = sp // 2, sp % 2
    other = col * 2 + (1 - side)
    rows = tok.shape[1]
    heads, width = qg_ref.shape
    kv_heads = kg_ref.shape[0]
    share = heads // kv_heads
    count = rows * n_tp

    def across(i):
        return lax.rem(pair + i, pairs) * 2 + core

    kv_cols = wk_hbm.shape[0]
    loads = [
        pltpu.make_async_copy(src, dst, local_sem.at[i])
        for i, (src, dst) in enumerate(
            ((tok_hbm, tok.at[tp]), (wq_hbm, wq), (wk_hbm, wkv.at[0:kv_cols]), (wv_hbm, wkv.at[kv_cols:]), (wo_hbm, wo.at[core]))
        )
    ]
    for load in loads:
        load.start()

    barrier = pltpu.get_barrier_semaphore()
    peers = 0
    for i in range(1, pairs):
        pl.semaphore_signal(barrier, inc=1, device_id={"tp": across(i)}, device_id_type=MESH)
        peers += 1
    pl.semaphore_signal(barrier, inc=1, device_id={"tp": mate}, device_id_type=MESH)
    pl.semaphore_signal(barrier, inc=1, device_id={"sp": other}, device_id_type=MESH)
    peers += 2
    for i in range(1, cols):
        peer = lax.rem(col + i, cols) * 2 + side
        pl.semaphore_signal(barrier, inc=1, device_id={"sp": peer}, device_id_type=MESH)
        peers += 1
    pl.semaphore_wait(barrier, peers)

    def send(src, dst, send_sem, recv_sem, where):
        return pltpu.make_async_remote_copy(
            src_ref=src,
            dst_ref=dst,
            send_sem=send_sem,
            recv_sem=recv_sem,
            device_id=where,
            device_id_type=MESH,
        )

    pending = []

    def go(copy):
        copy.start()
        pending.append(copy)

    def token_copy(block, src, slot, target):
        return send(src, tok.at[block], tok_send.at[slot], tok_recv.at[block], {"tp": target})

    for i in range(1, pairs):
        go(token_copy(tp, tok_hbm, i, across(i)))
    go(token_copy(tp, tok_hbm, 0, mate))

    gains[...] = jnp.zeros_like(gains)
    gains[0:heads, 0:width] = qg_ref[...].astype(F32) * (LOG2E * width ** (-0.5))
    gains[heads : heads + kv_heads, 0:width] = kg_ref[...].astype(F32)
    turned_gains = jnp.transpose(gains[...])
    tables = angle_tables(sp * count, count, width // 4)
    top[...] = jnp.full_like(top, -1e30)
    acc[...] = jnp.zeros_like(acc)
    loads[2].wait()
    loads[3].wait()
    loads[1].wait()
    loads[0].wait()
    query_cols = wq.shape[1]

    def project(block):
        piece = tok[block]
        at = pl.ds(pl.multiple_of(block * rows, rows), rows)
        raw[at, 0:query_cols] = jnp.dot(piece, wq[...], preferred_element_type=F32)
        raw[at, query_cols:] = lax.dot_general(
            piece, wkv[...], (((1,), (1,)), ((), ())), preferred_element_type=F32
        )

    kv_rows = kv_heads * width
    span = 2 * rows

    def span_of(part):
        return pl.ds(pl.multiple_of(part * span, span), span)

    def make_kv(part):
        at = span_of(part)
        turned = jnp.transpose(raw[at, query_cols : query_cols + kv_rows])
        angles = angle_tables(sp * count + part * span, span, width // 4)
        for h in range(kv_heads):
            gain = turned_gains[0:width, heads + h : heads + h + 1]
            keys = prepare(turned[h * width : (h + 1) * width], gain, angles)
            kv[sp, at, h * width : (h + 1) * width] = jnp.transpose(keys).astype(BF16)
        kv[sp, at, kv_rows : 2 * kv_rows] = raw[at, query_cols + kv_rows :].astype(BF16)

    def kv_copy(block, part, slot, where):
        spot = kv.at[block, span_of(part)]
        return send(spot, spot, kv_send.at[slot, part], kv_recv.at[block, part], {"sp": where})

    def near(distance, act):
        for way in (1, -1):
            place = col + distance * way

            @pl.when(jnp.logical_and(place >= 0, place < cols))
            def _():
                act(place)

    def to_column(place, part):
        return kv_copy(sp, part, place, place * 2 + side)

    def to_other(place, part):
        return kv_copy(place * 2 + side, part, cols + place, other)

    def send_kv(part):
        to_other(col, part).start()
        for distance in range(1, cols):
            near(distance, lambda place: to_column(place, part).start())

    def forward(place, part):
        kv_copy(place * 2 + side, part, 0, other).wait_recv()
        to_other(place, part).start()

    project(tp)
    token_copy(mate, tok_hbm, 0, mate).wait_recv()
    project(mate)
    make_kv(pair)
    send_kv(pair)
    for i in range(1, pairs):
        block = across(i)
        token_copy(block, tok_hbm, i, block).wait_recv()
        go(token_copy(block, tok.at[block], pairs + i, mate))
        project(block)
    loads[4].wait()
    wo_copy = send(wo_hbm, wo.at[core], wo_send, wo_recv, {"tp": mate})
    wo_copy.start()
    for i in range(1, pairs):
        block = lax.rem(pair + i, pairs) * 2 + (1 - core)
        token_copy(block, tok_hbm, i, mate).wait_recv()
        project(block)
        part = lax.rem(pair + i, pairs)
        make_kv(part)
        send_kv(part)
    for distance in range(1, cols):
        near(distance, lambda place: forward(place, pair))

    turned = jnp.transpose(raw[:, 0:query_cols])
    for h in range(heads):
        q = prepare(turned[h * width : (h + 1) * width], turned_gains[0:width, h : h + 1], tables)
        queries[h] = q.astype(BF16)

    def attend(block):
        ones = jnp.ones((ONES, count), BF16)
        turned = jnp.transpose(kv[block])
        for g in range(kv_heads):
            keys = kv[block, :, g * width : (g + 1) * width]
            values = turned[kv_rows + g * width : kv_rows + (g + 1) * width]
            values = jnp.concatenate([values, ones], axis=0)
            for h in range(g * share, (g + 1) * share):
                scores = jnp.dot(keys, queries[h], preferred_element_type=F32)
                old = top[h : h + 1, :]
                new = jnp.maximum(old, jnp.max(scores, axis=0, keepdims=True))
                weights = jnp.exp2((scores - new).astype(BF16))
                mixed = jnp.dot(values, weights, preferred_element_type=F32)
                acc[h] = acc[h] * jnp.exp2(old - new) + mixed
                top[h : h + 1, :] = new

    def straight(place):
        for i in range(1, pairs):
            forward(place, lax.rem(pair + i, pairs))
        attend(place * 2 + side)

    def mirrored(place):
        block = place * 2 + (1 - side)
        for part in range(pairs):
            kv_copy(block, part, 0, other).wait_recv()
        attend(block)

    attend(sp)
    mirrored(col)

    def step(distance, carry):
        near(distance, straight)

        @pl.when(distance > 1)
        def _():
            near(distance - 1, mirrored)

        return carry

    lax.fori_loop(1, cols, step, 0)
    near(cols - 1, mirrored)

    finished = []
    for h in range(heads):
        total = acc[h, width : width + 1, :]
        finished.append(acc[h, 0:width, :] / total)
        log_ref[h : h + 1, :] = (top[h : h + 1, :] + jnp.log2(total)) * LN2
    attended = jnp.transpose(jnp.concatenate(finished, axis=0)).astype(BF16)
    for t in range(n_tp):
        piece = attended[t * rows : (t + 1) * rows]

        @pl.when(core == t % 2)
        def _():
            att_own[t // 2] = piece

        @pl.when(core != t % 2)
        def _():
            att_out[t // 2] = piece

    att_copy = send(att_out, att_in, att_send, att_recv, {"tp": mate})
    att_copy.start()
    att_copy.wait_recv()
    wo_copy.wait_recv()
    step_cols = mixed_ref.shape[1] // chunks

    def product(place, n):
        at = slice(n * step_cols, (n + 1) * step_cols)
        return jnp.dot(
            att_own[place], wo[core, :, at], preferred_element_type=F32
        ) + jnp.dot(att_in[place], wo[1 - core, :, at], preferred_element_type=F32)

    def part_copy(i, n):
        slot = (i - 1) * chunks + n
        return send(
            part_out.at[slot],
            part_in.at[slot],
            part_send.at[slot],
            part_recv.at[slot],
            {"tp": across(i)},
        )

    for n in range(chunks):
        for i in range(1, pairs):
            part_out[(i - 1) * chunks + n] = product(lax.rem(pair + i, pairs), n).astype(BF16)
            part_copy(i, n).start()
    for n in range(chunks):
        at = slice(n * step_cols, (n + 1) * step_cols)
        total = product(pair, n)
        for i in range(1, pairs):
            part_copy(i, n).wait_recv()
            total = total + part_in[(i - 1) * chunks + n].astype(F32)
        mixed_ref[:, at] = total.astype(BF16)

    for copy in pending:
        copy.wait_send()
    wo_copy.wait_send()
    att_copy.wait_send()
    for part in range(pairs):
        to_other(col, part).wait_send()
        for distance in range(1, cols):
            near(distance, lambda place: to_column(place, part).wait_send())
            near(distance, lambda place: to_other(place, part).wait_send())
    for n in range(chunks):
        for i in range(1, pairs):
            part_copy(i, n).wait_send()


def body(n_sp, n_tp, tokens, query_weight, key_weight, value_weight, out_weight, query_gain, key_gain):
    rows, depth = tokens.shape
    query_cols = query_weight.shape[1]
    kv_cols = key_weight.shape[1]
    heads, width = query_gain.shape
    kv_heads = key_gain.shape[0]
    group, model = out_weight.shape
    count = rows * n_tp
    pairs, cols = n_tp // 2, n_sp // 2
    chunks = 4
    any_space = pl.BlockSpec(memory_space=pl.ANY)
    vmem = pl.BlockSpec(memory_space=pltpu.VMEM)
    dma = pltpu.SemaphoreType.DMA
    slots = max(pairs - 1, 1) * chunks
    return pl.pallas_call(
        functools.partial(kernel, n_sp, n_tp, chunks),
        out_shape=(
            pltpu.VMEM((rows, model), BF16),
            pltpu.VMEM((heads, count), F32),
        ),
        in_specs=[any_space] * 5 + [vmem] * 2,
        out_specs=(vmem, vmem),
        scratch_shapes=[
            pltpu.VMEM((n_tp, rows, depth), BF16),
            pltpu.VMEM((depth, query_cols), BF16),
            pltpu.VMEM((2 * kv_cols, depth), BF16),
            pltpu.VMEM((2, group, model), BF16),
            pltpu.VMEM((128, 128), F32),
            pltpu.VMEM((count, query_cols + 2 * kv_cols), F32),
            pltpu.VMEM((heads, width, count), BF16),
            pltpu.VMEM((n_sp, count, 2 * kv_heads * width), BF16),
            pltpu.VMEM((heads, count), F32),
            pltpu.VMEM((heads, width + ONES, count), F32),
            pltpu.VMEM((pairs, rows, group), BF16),
            pltpu.VMEM((pairs, rows, group), BF16),
            pltpu.VMEM((pairs, rows, group), BF16),
            pltpu.VMEM((slots, rows, model // chunks), BF16),
            pltpu.VMEM((slots, rows, model // chunks), BF16),
            dma((5,)),
            dma((2 * pairs,)),
            dma((n_tp,)),
            dma,
            dma,
            dma((2 * cols, pairs)),
            dma((n_sp, pairs)),
            dma,
            dma,
            dma((slots,)),
            dma((slots,)),
        ],
        compiler_params=pltpu.CompilerParams(
            collective_id=0, has_side_effects=True, vmem_limit_bytes=60 * 1024 * 1024
        ),
        name="attention",
    )(tokens, query_weight, key_weight.T, value_weight.T, out_weight, query_gain, key_gain)


def solution(mesh):
    return jax.shard_map(
        functools.partial(body, mesh.shape["sp"], mesh.shape["tp"]),
        mesh=mesh,
        in_specs=(
            P(("sp", "tp"), None),
            P(None, "tp"),
            P(None, "tp"),
            P(None, "tp"),
            P("tp", None),
            P("tp", None),
            P("tp", None),
        ),
        out_specs=(P(("sp", "tp"), None), P("tp", "sp")),
        check_vma=False,
    )
```
